32 devices in a mesh: sp: 8 (over z, y), tp: 4 (over x, core).
Axes of the slice: x: 2, y: 2, z: 4, core: 2. Of those that a mesh axis runs over, the one named last changes fastest.
Arguments:
- query_first: bfloat16 [2048, 512], P('sp', 'tp'), may hold values from -6 to 6
- key_first: bfloat16 [2048, 512], P('sp', 'tp'), may hold values from -6 to 6
- value_first: bfloat16 [2048, 1024], P('sp', 'tp'), may hold values from -6 to 6
- decay_first: float32 [2048, 512], P('sp', 'tp'), may hold values from -1 to 0
- gate_first: bfloat16 [2048, 1024], P('sp', 'tp'), may hold values from -6 to 6
- norm_first: float32 [256], replicated, may hold values from 0.1 to 1.9
- proj_first: bfloat16 [1024, 2048], P('tp', 'sp'), may hold values from -0.125 to 0.125
- query_second: bfloat16 [2048, 512], P('sp', 'tp'), may hold values from -6 to 6
- key_second: bfloat16 [2048, 512], P('sp', 'tp'), may hold values from -6 to 6
- value_second: bfloat16 [2048, 1024], P('sp', 'tp'), may hold values from -6 to 6
- decay_second: float32 [2048, 512], P('sp', 'tp'), may hold values from -1 to 0
- gate_second: bfloat16 [2048, 1024], P('sp', 'tp'), may hold values from -6 to 6
- norm_second: float32 [128], replicated, may hold values from 0.1 to 1.9
- proj_second: bfloat16 [1024, 2048], P('tp', 'sp'), may hold values from -0.125 to 0.125
- residual_in: bfloat16 [2048, 2048], P(('sp', 'tp')), may hold values from -6 to 6
- expert_norm: float32 [2048], replicated, may hold values from 0.1 to 1.9
- route_ids: int32 [2048, 2], P('sp'), may hold values from 0 to 7, all different within a row; in each aligned block of 256 rows (0 to 255, 256 to 511, ...) at most 128 rows name the same one
- route_weight: float32 [2048, 2], P('sp'), may hold values from 0.1 to 0.9
- expert_gate: bfloat16 [8, 2048, 3584], P('sp', None, 'tp'), may hold values from -0.125 to 0.125
- expert_up: bfloat16 [8, 2048, 3584], P('sp', None, 'tp'), may hold values from -0.125 to 0.125
- expert_down: bfloat16 [8, 3584, 2048], P('sp', 'tp'), may hold values from -0.09375 to 0.09375
Outputs:
- layer_out: bfloat16 [2048, 2048], P(('sp', 'tp'))
The draws below stay inside these ranges and needn't reach their ends.
Inputs may be any that keep to these rules, and one draw needn't show every extreme that they name: `route_ids`: each row names 2 different experts. Among the 256 rows of one index of sp no expert is named by more than 128 rows, and in every draw some expert is named by exactly 128 of them.
All inputs are finite; a program needn't handle non-finite values.
Results may differ from the reference program's by a relative error of at most 0.015.
Values may be sent and summed in bfloat16 or wider, within the bound.
A program may use at most 64 MiB of HBM per device.

```python
import math
import jax
import jax.numpy as jnp
import numpy as np
from jax import lax

D = 2048
FF = 3584
HEADS_A = 4
KA = 128
VA = 256
HEADS_B = 8
KB = 64
VB = 128
TOPK = 2
BLK = 64
TOK_DEV = 256
TOKENS = 2048
EXPERTS = 8
CAP = 128
N_TP = 4


def decay_draw(key, count_of_tokens, feature_channels):
    random_subkeys = jax.random.split(key, 7)
    slow_share = 0.5
    gradual_mask = jax.random.uniform(random_subkeys[0], (feature_channels,), jnp.float32) < slow_share
    fast_rates = jnp.exp(jax.random.uniform(random_subkeys[1], (feature_channels,), jnp.float32, jnp.log(1.0 / 60.0), jnp.log(1.0 / 30.0)))
    slow_rates = jnp.exp(jax.random.uniform(random_subkeys[2], (feature_channels,), jnp.float32, jnp.log(0.05 / count_of_tokens), jnp.log(0.3 / count_of_tokens)))
    rates = jnp.where(gradual_mask, slow_rates, fast_rates)
    shard_factor = jnp.exp(jax.random.uniform(random_subkeys[3], (count_of_tokens // TOK_DEV,), jnp.float32, jnp.log(0.5), jnp.log(2.0)))
    shard_factor = jnp.repeat(shard_factor, TOK_DEV)
    roughness = jnp.exp(0.5 * jnp.clip(jax.random.normal(random_subkeys[4], (count_of_tokens, feature_channels), jnp.float32), -2.5, 2.5))
    decay_factors = -rates[None, :] * shard_factor[:, None] * roughness
    spike_position = jax.random.randint(random_subkeys[5], (3,), 0, count_of_tokens)
    spike_found = jnp.any(jnp.arange(count_of_tokens)[:, None] == spike_position[None, :], axis=1)
    spike_penalty = jnp.log(jax.random.uniform(random_subkeys[6], (feature_channels,), jnp.float32, 0.6, 0.8))
    decay_factors = decay_factors + jnp.where(spike_found[:, None] & gradual_mask[None, :], spike_penalty[None, :], 0.0)
    return decay_factors.astype(jnp.float32)


def draw_decay_first(key, part):
    return decay_draw(jax.random.fold_in(key, 11), TOKENS, HEADS_A * KA)


def draw_decay_second(key, part):
    return decay_draw(jax.random.fold_in(key, 23), TOKENS, HEADS_B * KB)


def block_levels(stream_key, extent, shards, low, top_value):
    def one(axis_at, parts):
        draws = jax.random.uniform(jax.random.fold_in(jax.random.fold_in(stream_key, 6), axis_at), (parts,), jnp.float32, low / len(shards), top_value / len(shards))
        return jnp.repeat(jnp.exp(draws), extent[axis_at] // parts).reshape((-1,) + (1,) * (len(extent) - axis_at - 1))

    factor_of = one(*shards[0])
    for cut in shards[1:]:
        factor_of = factor_of * one(*cut)
    return factor_of


def routed_block(rng, own, number, rows, amount, top, most, skew):
    order = jax.random.permutation(rng, amount)
    packed, ordinary = load_shares(amount, rows * top, most, skew, True), load_shares(amount, rows * top, most, skew, False)
    places = jnp.arange(amount)

    def named(sizes, offset_by):
        used = int((sizes > 0).sum())
        fixed = max(1, used // 4)
        shifted = fixed + (places - fixed + offset_by * (used - fixed)) % max(1, amount - fixed)
        return jnp.zeros((amount,), jnp.int32).at[order[jnp.where(places < fixed, places, shifted)]].set(jnp.asarray(sizes, jnp.int32))

    sizes = jnp.where(number % 4 == 0, named(packed, number // 4), named(ordinary, number - number // 4 - 1))
    mixed = jax.random.permutation(jax.random.fold_in(own, 3), amount)
    giver, receiver = mixed[0:amount // 2 * 2:2], mixed[1:amount // 2 * 2:2]
    slack = jnp.minimum(sizes[giver] - 1, most - sizes[receiver]) // 2
    slack = jnp.where((giver == order[0]) | (receiver == order[0]) | (sizes[receiver] == 0), 0, jnp.maximum(slack, 0))
    shifted = jax.random.randint(jax.random.fold_in(own, 4), (amount // 2,), 0, 1 << 20) % (slack + 1)
    sizes = sizes.at[giver].add(-shifted).at[receiver].add(shifted)
    labels = jnp.searchsorted(jnp.cumsum(sizes), jnp.arange(rows * top), side="right").astype(jnp.int32)
    grid = labels.reshape(top, rows).T
    grid = grid[jax.random.permutation(jax.random.fold_in(own, 1), rows)]
    offset_by = jax.random.randint(jax.random.fold_in(own, 2), (rows, 1), 0, top)
    return jnp.take_along_axis(grid, (jnp.arange(top)[None, :] + offset_by) % top, axis=1)


def load_shares(amount, total, most, skew, full):
    portions = [(1 << 20) // math.isqrt(grade ** skew) + 1 for grade in range(1, amount + 1)]
    largest = most if full else min(most, max(-(-total // amount), total * portions[0] // sum(portions)))
    least = 1 if total - largest >= amount - 1 else 0
    holding, surplus = [largest] + [least] * (amount - 1), total - largest - least * (amount - 1)
    while surplus > 0:
        candidates = [i for i in range(1, amount) if holding[i] < largest] or [i for i in range(1, amount) if holding[i] < most]
        mass, remaining = sum([portions[i] for i in candidates]), surplus
        for i in candidates:
            more = min(most - holding[i], max(1, remaining * portions[i] // mass), surplus)
            holding[i] = holding[i] + more
            surplus = surplus - more
    return np.array(holding)


def scatter_about(own_key, shape, deviation, reach, shards=(), held_as=jnp.bfloat16):
    gain = block_levels(own_key, shape, shards, -0.22, 0.18) if shards else 1.0
    entries = jax.random.normal(own_key, shape, jnp.float32) * deviation * gain
    return jnp.minimum(jnp.maximum(entries, -reach), reach).astype(held_as)


def setup_inputs(seed: int = 0) -> dict:
    arg_keys = jax.random.split(jax.random.key(seed), 22)
    query_first = scatter_about(arg_keys[0], (TOKENS, HEADS_A * KA), 1.0, 6.0, ((0, 8), (1, 4)))
    key_first = scatter_about(arg_keys[1], (TOKENS, HEADS_A * KA), 1.0, 6.0, ((0, 8), (1, 4)))
    value_first = scatter_about(arg_keys[2], (TOKENS, HEADS_A * VA), 1.0, 6.0, ((0, 8), (1, 4)))
    decay_first = draw_decay_first(jax.random.fold_in(arg_keys[21], 71), 0)
    gate_first = scatter_about(arg_keys[4], (TOKENS, HEADS_A * VA), 1.0, 6.0, ((0, 8), (1, 4)))
    norm_first = jnp.clip(1.0 + 0.18 * jax.random.normal(arg_keys[5], (VA,), jnp.float32), 0.1, 1.9)
    proj_first = scatter_about(arg_keys[6], (HEADS_A * VA, D), (HEADS_A * VA + HEADS_B * VB) ** -0.5, 0.125, ((0, 4), (1, 8)))
    query_second = scatter_about(arg_keys[7], (TOKENS, HEADS_B * KB), 1.0, 6.0, ((0, 8), (1, 4)))
    key_second = scatter_about(arg_keys[8], (TOKENS, HEADS_B * KB), 1.0, 6.0, ((0, 8), (1, 4)))
    value_second = scatter_about(arg_keys[9], (TOKENS, HEADS_B * VB), 1.0, 6.0, ((0, 8), (1, 4)))
    decay_second = draw_decay_second(jax.random.fold_in(arg_keys[21], 71), 0)
    gate_second = scatter_about(arg_keys[11], (TOKENS, HEADS_B * VB), 1.0, 6.0, ((0, 8), (1, 4)))
    norm_second = jnp.clip(1.0 + 0.18 * jax.random.normal(arg_keys[12], (VB,), jnp.float32), 0.1, 1.9)
    proj_second = scatter_about(arg_keys[13], (HEADS_B * VB, D), (HEADS_A * VA + HEADS_B * VB) ** -0.5, 0.125, ((0, 4), (1, 8)))
    residual_in = scatter_about(arg_keys[14], (TOKENS, D), 1.0, 6.0, ((0, 32),))
    expert_norm = jnp.clip(1.0 + 0.18 * jax.random.normal(arg_keys[15], (D,), jnp.float32), 0.1, 1.9)
    route_ids_keys = jax.random.split(jax.random.fold_in(arg_keys[16], 1), TOKENS // TOK_DEV)
    route_ids_turns = jax.random.permutation(jax.random.fold_in(arg_keys[16], 3), TOKENS // TOK_DEV)
    route_ids = jax.vmap(lambda own, number: routed_block(jax.random.fold_in(arg_keys[16], 2), own, number, TOK_DEV, EXPERTS, TOPK, CAP, 1))(route_ids_keys, route_ids_turns).reshape((TOKENS, TOPK))
    route_weight = jnp.clip(0.1 + 0.79999997 * jax.random.uniform(arg_keys[17], (TOKENS, TOPK), jnp.float32) ** block_levels(arg_keys[17], (TOKENS, TOPK), ((0, 8),), -0.2, 0.2), 0.1, 0.9)
    expert_gate = scatter_about(arg_keys[18], (EXPERTS, D, FF), D ** -0.5, 0.125, ((0, 8), (2, 4)))
    expert_up = scatter_about(arg_keys[19], (EXPERTS, D, FF), D ** -0.5, 0.125, ((0, 8), (2, 4)))
    expert_down = scatter_about(arg_keys[20], (EXPERTS, FF, D), FF ** -0.5, 0.09375, ((0, 8), (1, 4)))
    return dict(query_first=query_first, key_first=key_first, value_first=value_first, decay_first=decay_first, gate_first=gate_first, norm_first=norm_first, proj_first=proj_first, query_second=query_second, key_second=key_second, value_second=value_second, decay_second=decay_second, gate_second=gate_second, norm_second=norm_second, proj_second=proj_second, residual_in=residual_in, expert_norm=expert_norm, route_ids=route_ids, route_weight=route_weight, expert_gate=expert_gate, expert_up=expert_up, expert_down=expert_down)


epsilon = 1e-06
highest = lax.Precision.HIGHEST

def attend(queries, key_rows, values, decay_factors, key_width, value_width):
    count_of_tokens = queries.shape[0]
    head_count = queries.shape[1] // key_width
    blocks = count_of_tokens // BLK

    def arrange(source, feature_channels):
        return source.astype(jnp.float32).reshape(blocks, BLK, head_count, feature_channels).transpose(0, 2, 1, 3)
    causal = jnp.tril(jnp.ones((BLK, BLK), jnp.float32))

    def block_step(carry_state, inputs):
        query_block, key_block, value_block, decay_block = inputs
        cumulative = jnp.cumsum(decay_block, axis=1)
        block_end = cumulative[:, -1:, :]
        query_decayed = query_block * jnp.exp(cumulative)
        key_inverse = key_block * jnp.exp(-cumulative)
        key_to_end = key_block * jnp.exp(block_end - cumulative)
        scores = jnp.einsum('htd,hsd->hts', query_decayed, key_inverse, precision=highest) * causal
        outputs = jnp.einsum('hts,hsv->htv', scores, value_block, precision=highest)
        outputs = outputs + jnp.einsum('htd,hdv->htv', query_decayed, carry_state, precision=highest)
        carry_state = jnp.exp(block_end)[:, 0, :, None] * carry_state + jnp.einsum('hsd,hsv->hdv', key_to_end, value_block, precision=highest)
        return (carry_state, outputs)
    start_state = jnp.zeros((head_count, key_width, value_width), jnp.float32)
    scaled = arrange(queries, key_width) * key_width ** (-0.5)
    end_state, outputs = lax.scan(block_step, start_state, (scaled, arrange(key_rows, key_width), arrange(values, value_width), arrange(decay_factors, key_width)))
    return outputs.transpose(0, 2, 1, 3).reshape(count_of_tokens, head_count, value_width)

def head_norm(attention, head_gain, gate):
    inverse_rms = lax.rsqrt(lax.optimization_barrier(jnp.mean(attention * attention, axis=-1, keepdims=True)) + epsilon)
    gate_silu = jax.nn.silu(gate.astype(jnp.float32).reshape(attention.shape))
    mixed_rows = attention * inverse_rms * head_gain.astype(jnp.float32) * gate_silu
    return mixed_rows.astype(jnp.bfloat16).reshape(attention.shape[0], -1)

def route_tables(block_routes):
    flattened = block_routes.reshape(-1)
    onehot = (flattened[:, None] == jnp.arange(EXPERTS, dtype=jnp.int32)[None, :]).astype(jnp.int32)
    before = (jnp.cumsum(onehot, axis=0) - onehot).astype(jnp.int32)
    ranking = lax.optimization_barrier(jnp.sum(before * onehot, axis=1)).astype(jnp.int32)
    slot_ids = (flattened * CAP + ranking).astype(jnp.int32)
    row_token = (jnp.arange(TOK_DEV * TOPK, dtype=jnp.int32) // TOPK).astype(jnp.int32)
    owners = jnp.full((EXPERTS * CAP,), TOK_DEV, jnp.int32).at[slot_ids].set(row_token)
    return (owners, slot_ids)

def place_weights(slot_ids, weights):
    return jnp.zeros((EXPERTS * CAP,), jnp.float32).at[slot_ids].set(weights.astype(jnp.float32))

def pick_rows(block_rows, index_list):
    return jnp.take(block_rows, index_list, axis=0)

def reference(query_first, key_first, value_first, decay_first, gate_first, norm_first, proj_first, query_second, key_second, value_second, decay_second, gate_second, norm_second, proj_second, residual_in, expert_norm, route_ids, route_weight, expert_gate, expert_up, expert_down):
    attention_first = attend(query_first, key_first, value_first, decay_first, KA, VA)
    attention_second = attend(query_second, key_second, value_second, decay_second, KB, VB)
    mixed_first = head_norm(attention_first, norm_first, gate_first)
    mixed_second = head_norm(attention_second, norm_second, gate_second)
    rows_first = HEADS_A // N_TP * VA
    rows_second = HEADS_B // N_TP * VB
    mixture = jnp.zeros((TOKENS, D), jnp.float32)
    for portion in range(N_TP):
        portion_sum = jnp.dot(mixed_first[:, portion * rows_first:(portion + 1) * rows_first], proj_first[portion * rows_first:(portion + 1) * rows_first], preferred_element_type=jnp.float32)
        portion_sum = portion_sum + jnp.dot(mixed_second[:, portion * rows_second:(portion + 1) * rows_second], proj_second[portion * rows_second:(portion + 1) * rows_second], preferred_element_type=jnp.float32)
        rounded = lax.optimization_barrier(portion_sum.astype(jnp.bfloat16))
        mixture = mixture + rounded.astype(jnp.float32)
    residual = (residual_in.astype(jnp.float32) + mixture).astype(jnp.bfloat16)
    as_float = residual.astype(jnp.float32)
    inverse_rms = lax.rsqrt(lax.optimization_barrier(jnp.mean(as_float * as_float, axis=-1, keepdims=True)) + epsilon)
    normed = (as_float * inverse_rms * expert_norm.astype(jnp.float32)).astype(jnp.bfloat16)
    block_count = TOKENS // TOK_DEV
    owners, slot_ids = jax.vmap(route_tables)(route_ids.reshape(block_count, TOK_DEV, TOPK))
    slot_weight = jax.vmap(place_weights)(slot_ids, route_weight.reshape(block_count, TOK_DEV * TOPK))
    padded = jnp.concatenate((normed.reshape(block_count, TOK_DEV, D), jnp.zeros((block_count, 1, D), jnp.bfloat16)), axis=1)
    block_base = (jnp.arange(block_count, dtype=jnp.int32) * TOK_DEV).astype(jnp.int32)[:, None]
    quarter_width = FF // N_TP

    def expert_step(combined, inputs):
        gate_matrix, up_matrix, down_matrix, expert = inputs
        chosen = lax.dynamic_slice_in_dim(owners, (expert * CAP).astype(jnp.int32), CAP, 1)
        gathered = jax.vmap(pick_rows)(padded, chosen)
        flattened = gathered.reshape(block_count * CAP, D)
        gate_part = jnp.dot(flattened, gate_matrix, preferred_element_type=jnp.float32)
        up_part = jnp.dot(flattened, up_matrix, preferred_element_type=jnp.float32)
        hidden = (jax.nn.silu(gate_part) * up_part).astype(jnp.bfloat16)
        summed = jnp.zeros((block_count * CAP, D), jnp.float32)
        for portion in range(N_TP):
            piece = jnp.dot(hidden[:, portion * quarter_width:(portion + 1) * quarter_width], down_matrix[portion * quarter_width:(portion + 1) * quarter_width], preferred_element_type=jnp.float32)
            rounded = lax.optimization_barrier(piece.astype(jnp.bfloat16))
            summed = summed + rounded.astype(jnp.float32)
        weights_here = lax.dynamic_slice_in_dim(slot_weight, (expert * CAP).astype(jnp.int32), CAP, 1).reshape(-1, 1)
        targets = jnp.where(chosen == TOK_DEV, TOKENS, block_base + chosen).astype(jnp.int32).reshape(-1)
        combined = combined.at[targets].add(summed * weights_here)
        return (combined, None)
    combined_start = jnp.zeros((TOKENS + 1, D), jnp.float32)
    combined, _ = lax.scan(expert_step, combined_start, (expert_gate, expert_up, expert_down, jnp.arange(EXPERTS, dtype=jnp.int32)))
    return (residual.astype(jnp.float32) + combined[:TOKENS]).astype(jnp.bfloat16)
```

```python
import functools

import jax
import jax.numpy as jnp
from jax import lax
from jax.experimental import pallas as pl
from jax.experimental.pallas import tpu as pltpu
from jax.sharding import PartitionSpec as P

KA = 128
VA = 256
KB = 64
VB = 128
BLK = 64
PAIR = 2


epsilon = 1e-06
highest = lax.Precision.HIGHEST
MESH = pl.DeviceIdType.MESH
VMEM = pl.BlockSpec(memory_space=pltpu.VMEM)


def greet(peers):
    barrier = pltpu.get_barrier_semaphore()
    for peer in peers:
        pl.semaphore_signal(barrier, inc=1, device_id=peer, device_id_type=MESH)
    pl.semaphore_wait(barrier, len(peers))


def group_member(axis, span, step):
    me = lax.axis_index(axis)
    inside = lax.rem(me, span)
    other = lax.rem(inside + step, span)
    return inside, other, {axis: me - inside + other}


def exchange_kernel(axis, span, spread, count, *refs):
    sources, targets = refs[:count], refs[count : 2 * count]
    send_sems, recv_sems = refs[2 * count :]
    greet([group_member(axis, span, step)[2] for step in range(1, span)])
    copies = []
    for step in range(1, span):
        inside, other, device = group_member(axis, span, step)
        for i in range(count):
            copy = pltpu.make_async_remote_copy(
                src_ref=sources[i].at[other] if spread else sources[i],
                dst_ref=targets[i].at[inside],
                send_sem=send_sems.at[i, step],
                recv_sem=recv_sems.at[i, step],
                device_id=device,
                device_id_type=MESH,
            )
            copy.start()
            copies.append(copy)
    inside = lax.rem(lax.axis_index(axis), span)
    for i in range(count):
        targets[i][inside] = sources[i][inside] if spread else sources[i][...]
    for copy in copies:
        copy.wait()


def exchange(arrays, axis, span, spread, number):
    shapes = tuple(
        jax.ShapeDtypeStruct(a.shape if spread else (span,) + a.shape, a.dtype) for a in arrays
    )
    count = len(arrays)
    return pl.pallas_call(
        functools.partial(exchange_kernel, axis, span, spread, count),
        out_shape=shapes,
        in_specs=[VMEM] * count,
        out_specs=(VMEM,) * count,
        scratch_shapes=[
            pltpu.SemaphoreType.DMA((count, span)),
            pltpu.SemaphoreType.DMA((count, span)),
        ],
        compiler_params=pltpu.CompilerParams(collective_id=number, has_side_effects=True),
    )(*arrays)


def dispatch_kernel(size, source, target, send_sems, recv_sems, pair_send, pair_recv):
    half = lax.rem(lax.axis_index("tp"), PAIR)
    sibling = group_member("tp", PAIR, 1)[2]
    peers = [group_member("sp", size, step) for step in range(1, size)]
    greet([peer[2] for peer in peers] + [sibling])
    copies, forwards = [], []
    for step, (me, other, device) in enumerate(peers, 1):
        copy = pltpu.make_async_remote_copy(
            src_ref=source.at[other],
            dst_ref=target.at[half, me],
            send_sem=send_sems.at[step],
            recv_sem=recv_sems.at[step],
            device_id=device,
            device_id_type=MESH,
        )
        copy.start()
        copies.append(copy)
    me = lax.axis_index("sp")
    own = pltpu.make_async_remote_copy(
        src_ref=source.at[me],
        dst_ref=target.at[half, me],
        send_sem=pair_send.at[0],
        recv_sem=pair_recv.at[0],
        device_id=sibling,
        device_id_type=MESH,
    )
    own.start()
    forwards.append(own)
    target[half, me] = source[me]
    for step in range(1, size):
        copies[step - 1].wait_recv()
        origin = lax.rem(me - step + size, size)
        forward = pltpu.make_async_remote_copy(
            src_ref=target.at[half, origin],
            dst_ref=target.at[half, origin],
            send_sem=pair_send.at[step],
            recv_sem=pair_recv.at[step],
            device_id=sibling,
            device_id_type=MESH,
        )
        forward.start()
        forwards.append(forward)
    for copy in copies:
        copy.wait_send()
    for forward in forwards:
        forward.wait()


def dispatch(outgoing, number):
    size = outgoing.shape[0]
    return pl.pallas_call(
        functools.partial(dispatch_kernel, size),
        out_shape=jax.ShapeDtypeStruct((PAIR,) + outgoing.shape, outgoing.dtype),
        in_specs=[VMEM],
        out_specs=VMEM,
        scratch_shapes=[pltpu.SemaphoreType.DMA((size,)) for _ in range(4)],
        compiler_params=pltpu.CompilerParams(collective_id=number, has_side_effects=True),
    )(outgoing)


def local_pass(queries, key_rows, values, decay_factors, key_width, value_width):
    count_of_tokens = queries.shape[0]
    head_count = queries.shape[1] // key_width
    blocks = count_of_tokens // BLK
    lower = jnp.tril(jnp.ones((BLK, BLK), jnp.float32))

    def arrange(source, feature_channels):
        return (
            source.astype(jnp.float32)
            .reshape(blocks, BLK, head_count, feature_channels)
            .transpose(0, 2, 1, 3)
        )

    query_blocks = arrange(queries, key_width) * key_width ** (-0.5)
    key_blocks = arrange(key_rows, key_width)
    value_blocks = arrange(values, value_width)
    cumulative = jnp.einsum("ts,nhsd->nhtd", lower, arrange(decay_factors, key_width), precision=highest)
    block_end = cumulative[:, :, -1:, :]
    query_decayed = query_blocks * jnp.exp(cumulative)
    key_inverse = key_blocks * jnp.exp(-cumulative)
    key_to_end = key_blocks * jnp.exp(block_end - cumulative)
    scores = jnp.einsum("nhtd,nhsd->nhts", query_decayed, key_inverse, precision=highest) * lower
    inner = jnp.einsum("nhts,nhsv->nhtv", scores, value_blocks, precision=highest)
    added = jnp.einsum("nhsd,nhsv->nhdv", key_to_end, value_blocks, precision=highest)
    state = jnp.zeros((head_count, key_width, value_width), jnp.float32)
    states = []
    for n in range(blocks):
        states.append(state)
        state = jnp.exp(block_end[n, :, 0])[:, :, None] * state + added[n]
    ends = block_end[:, :, 0]
    return (query_decayed, inner, jnp.stack(states), ends, state)


def finish_pass(query_decayed, inner, states, ends, entering):
    before = jnp.cumsum(ends, axis=0) - ends
    states = states + jnp.exp(before)[:, :, :, None] * entering[None]
    out = inner + jnp.einsum("nhtd,nhdv->nhtv", query_decayed, states, precision=highest)
    blocks, heads, rows, width = out.shape
    return out.transpose(0, 2, 1, 3).reshape(blocks * rows, heads, width)


def entering_state(totals, states, index):
    size = totals.shape[0]
    k = jnp.arange(size)
    reached = (k < index)[:, None]
    masked = jnp.where(reached, totals, 0.0)
    after = (k[None, :] > k[:, None]).astype(jnp.float32)
    behind = jnp.sum(after[:, :, None] * masked[None], axis=1)
    factor = jnp.where(reached, jnp.exp(behind), 0.0)
    return jnp.sum(factor[:, :, None] * states.astype(jnp.float32), axis=0)


def head_norm(attention, head_gain, gate):
    inverse_rms = lax.rsqrt(jnp.mean(attention * attention, axis=-1, keepdims=True) + epsilon)
    gate_silu = jax.nn.silu(gate.astype(jnp.float32).reshape(attention.shape))
    mixed_rows = attention * inverse_rms * head_gain * gate_silu
    return mixed_rows.astype(jnp.bfloat16).reshape(attention.shape[0], -1)


def rms_scale(residual, gain_vector):
    as_float = residual.astype(jnp.float32)
    inverse_rms = lax.rsqrt(jnp.mean(as_float * as_float, axis=-1, keepdims=True) + epsilon)
    return (as_float * inverse_rms * gain_vector).astype(jnp.bfloat16)


def route_positions(block_routes, experts):
    flattened = block_routes.reshape(-1)
    amount = flattened.shape[0]
    onehot = flattened[:, None] == jnp.arange(experts, dtype=jnp.int32)[None, :]
    earlier = jnp.tril(jnp.ones((amount, amount), jnp.bfloat16), -1)
    before = jnp.dot(earlier, onehot.astype(jnp.bfloat16), preferred_element_type=jnp.float32)
    ranking = jnp.sum(jnp.where(onehot, before, 0.0), axis=1).astype(jnp.int32)
    return ranking.reshape(block_routes.shape)


def add_all(parts):
    return jnp.sum(parts.astype(jnp.float32), axis=0)


def shards(
    query_first,
    key_first,
    value_first,
    decay_first,
    gate_first,
    norm_first,
    proj_first,
    query_second,
    key_second,
    value_second,
    decay_second,
    gate_second,
    norm_second,
    proj_second,
    residual_in,
    expert_norm,
    route_ids,
    route_weight,
    expert_gate,
    expert_up,
    expert_down,
):
    sp_size, tp_size = lax.axis_size("sp"), lax.axis_size("tp")
    sp_index, tp_index = lax.axis_index("sp"), lax.axis_index("tp")
    projection = jnp.concatenate((proj_first, proj_second), axis=0)
    projection = lax.all_gather(projection, "sp", axis=1, tiled=True)

    first = local_pass(query_first, key_first, value_first, decay_first, KA, VA)
    second = local_pass(query_second, key_second, value_second, decay_second, KB, VB)
    total_first = jnp.sum(first[3], axis=0).reshape(1, -1)
    total_second = jnp.sum(second[3], axis=0).reshape(1, -1)
    totals = jnp.concatenate((total_first, total_second), axis=1)
    totals = jnp.broadcast_to(totals, (8, totals.shape[1]))
    all_totals, all_first, all_second = exchange(
        (
            totals,
            first[4].reshape(-1, VA).astype(jnp.bfloat16),
            second[4].reshape(-1, VB).astype(jnp.bfloat16),
        ),
        "sp",
        sp_size,
        False,
        0,
    )
    cut = total_first.shape[1]
    enter_first = entering_state(all_totals[:, 0, :cut], all_first, sp_index)
    enter_second = entering_state(all_totals[:, 0, cut:], all_second, sp_index)
    attention_first = finish_pass(*first[:4], enter_first.reshape(first[4].shape))
    attention_second = finish_pass(*second[:4], enter_second.reshape(second[4].shape))
    mixed_first = head_norm(attention_first, norm_first, gate_first)
    mixed_second = head_norm(attention_second, norm_second, gate_second)
    mixed_rows = jnp.concatenate((mixed_first, mixed_second), axis=1)
    partial_terms = jnp.dot(mixed_rows, projection, preferred_element_type=jnp.float32)
    block_tokens, top_count = route_ids.shape
    model_width = partial_terms.shape[1]
    own_tokens = block_tokens // tp_size
    (portions,) = exchange(
        (partial_terms.astype(jnp.bfloat16).reshape(tp_size, own_tokens, model_width),),
        "tp",
        tp_size,
        True,
        1,
    )
    residual = (residual_in.astype(jnp.float32) + add_all(portions)).astype(jnp.bfloat16)
    normed = rms_scale(residual, expert_norm)
    (gathered,) = exchange((normed,), "tp", tp_size, False, 2)
    gathered = gathered.reshape(block_tokens, model_width)

    experts = sp_size
    capacity = 2 * top_count * block_tokens // experts
    half = capacity // PAIR
    slots = experts * half
    place = route_positions(route_ids, experts) - lax.rem(tp_index, PAIR) * half
    local = jnp.where((place >= 0) & (place < half), route_ids * half + place, -1)
    numbers = jnp.arange(slots, dtype=jnp.int32)
    chosen, weights = (False, 0.0)
    for c in range(top_count):
        chosen = chosen | (numbers[:, None] == local[None, :, c])
        weights = weights + jnp.where(
            numbers[None, :] == local[:, c, None], route_weight[:, c, None], 0.0
        )
    outgoing = jnp.dot(
        chosen.astype(jnp.bfloat16), gathered, preferred_element_type=jnp.float32
    ).astype(jnp.bfloat16)
    incoming = dispatch(outgoing.reshape(experts, half, model_width), 3)
    incoming = incoming.reshape(-1, model_width)
    gate_part = jnp.dot(incoming, expert_gate[0], preferred_element_type=jnp.float32)
    up_part = jnp.dot(incoming, expert_up[0], preferred_element_type=jnp.float32)
    hidden = (jax.nn.silu(gate_part) * up_part).astype(jnp.bfloat16)
    produced = jnp.dot(hidden, expert_down[0], preferred_element_type=jnp.float32)
    produced = produced.astype(jnp.bfloat16).reshape(PAIR, slots, model_width)
    (halves,) = exchange((produced,), "tp", PAIR, True, 4)
    summed = add_all(halves).astype(jnp.bfloat16).reshape(experts, half, model_width)
    (returned,) = exchange((summed,), "sp", sp_size, True, 5)
    returned = returned.reshape(slots, model_width)
    coarse = weights.astype(jnp.bfloat16)
    fine = (weights - coarse.astype(jnp.float32)).astype(jnp.bfloat16)
    weighted = jnp.dot(coarse, returned, preferred_element_type=jnp.float32)
    weighted = weighted + jnp.dot(fine, returned, preferred_element_type=jnp.float32)
    (shares,) = exchange(
        (weighted.astype(jnp.bfloat16).reshape(tp_size, own_tokens, model_width),),
        "tp",
        tp_size,
        True,
        6,
    )
    return (residual.astype(jnp.float32) + add_all(shares)).astype(jnp.bfloat16)


def solution(mesh):
    in_specs = (
        P("sp", "tp"),
        P("sp", "tp"),
        P("sp", "tp"),
        P("sp", "tp"),
        P("sp", "tp"),
        P(),
        P("tp", "sp"),
        P("sp", "tp"),
        P("sp", "tp"),
        P("sp", "tp"),
        P("sp", "tp"),
        P("sp", "tp"),
        P(),
        P("tp", "sp"),
        P(("sp", "tp"), None),
        P(),
        P("sp", None),
        P("sp", None),
        P("sp", None, "tp"),
        P("sp", None, "tp"),
        P("sp", "tp", None),
    )
    out_specs = P(("sp", "tp"), None)
    return jax.shard_map(shards, mesh=mesh, in_specs=in_specs, out_specs=out_specs, check_vma=False)
```

```python
import functools

import jax
import jax.numpy as jnp
from jax import lax
from jax.experimental import pallas as pl
from jax.experimental.pallas import tpu as pltpu
from jax.sharding import PartitionSpec as P

KA = 128
VA = 256
KB = 64
VB = 128
BLK = 64
PAIR = 2


epsilon = 1e-06
highest = lax.Precision.HIGHEST
MESH = pl.DeviceIdType.MESH
VMEM = pl.BlockSpec(memory_space=pltpu.VMEM)


def greet(peers):
    barrier = pltpu.get_barrier_semaphore()
    for peer in peers:
        pl.semaphore_signal(barrier, inc=1, device_id=peer, device_id_type=MESH)
    pl.semaphore_wait(barrier, len(peers))


def group_member(axis, span, step):
    me = lax.axis_index(axis)
    inside = lax.rem(me, span)
    other = lax.rem(inside + step, span)
    return inside, other, {axis: me - inside + other}


def exchange_kernel(axis, span, spread, count, *refs):
    sources, targets = refs[:count], refs[count : 2 * count]
    send_sems, recv_sems = refs[2 * count :]
    greet([group_member(axis, span, step)[2] for step in range(1, span)])
    copies = []
    for step in range(1, span):
        inside, other, device = group_member(axis, span, step)
        for i in range(count):
            copy = pltpu.make_async_remote_copy(
                src_ref=sources[i].at[other] if spread else sources[i],
                dst_ref=targets[i].at[inside],
                send_sem=send_sems.at[i, step],
                recv_sem=recv_sems.at[i, step],
                device_id=device,
                device_id_type=MESH,
            )
            copy.start()
            copies.append(copy)
    inside = lax.rem(lax.axis_index(axis), span)
    for i in range(count):
        targets[i][inside] = sources[i][inside] if spread else sources[i][...]
    for copy in copies:
        copy.wait()


def exchange(arrays, axis, span, spread, number):
    shapes = tuple(
        jax.ShapeDtypeStruct(a.shape if spread else (span,) + a.shape, a.dtype) for a in arrays
    )
    count = len(arrays)
    return pl.pallas_call(
        functools.partial(exchange_kernel, axis, span, spread, count),
        out_shape=shapes,
        in_specs=[VMEM] * count,
        out_specs=(VMEM,) * count,
        scratch_shapes=[
            pltpu.SemaphoreType.DMA((count, span)),
            pltpu.SemaphoreType.DMA((count, span)),
        ],
        compiler_params=pltpu.CompilerParams(collective_id=number, has_side_effects=True),
    )(*arrays)


def tp_member(across, sibling):
    size, me = lax.axis_size("tp"), lax.axis_index("tp")
    seat = lax.rem(me, PAIR)
    base = lax.rem(me - seat + across * PAIR, size)
    return base + (lax.rem(seat + 1, PAIR) if sibling else seat)


def remote(source, target, sems, index, device):
    return pltpu.make_async_remote_copy(
        src_ref=source,
        dst_ref=target,
        send_sem=sems[0].at[index],
        recv_sem=sems[1].at[index],
        device_id=device,
        device_id_type=MESH,
    )


def gather_kernel(size, pairs, spread, source, target, *sems):
    sp_sems, pair_sems, far_sems = sems[:2], sems[2:4], sems[4:]
    me, mine = lax.axis_index("sp"), lax.axis_index("tp")
    sibling = {"tp": tp_member(0, True)}
    far = [{"tp": tp_member(across, False)} for across in range(1, pairs)]
    peers = [group_member("sp", size, step) for step in range(1, size)] if spread else []
    greet([peer[2] for peer in peers] + [sibling] + far)
    copies = []
    for step, (_, other, device) in enumerate(peers, 1):
        copies.append(remote(source.at[other], target.at[mine, me], sp_sems, step, device))
        copies[-1].start()
    passed, distant = [], []
    for step in range(size):
        if spread:
            origin = lax.rem(me - step + size, size)
        else:
            origin = step
        own = step == 0 or not spread
        if not own:
            copies[step - 1].wait_recv()
        block = source.at[origin] if own else target.at[mine, origin]
        for across in range(1, pairs):
            copy = remote(
                block, target.at[mine, origin], far_sems, (across, step), far[across - 1]
            )
            copy.start()
            distant.append((copy, tp_member(pairs - across, False), origin, across, step))
        copy = remote(block, target.at[mine, origin], pair_sems, (0, step), sibling)
        copy.start()
        passed.append(copy)
        if own:
            target[mine, origin] = source[origin]
    for copy, sender, origin, across, step in distant:
        copy.wait_recv()
        block = target.at[sender, origin]
        again = remote(block, block, pair_sems, (across, step), sibling)
        again.start()
        passed.append(again)
    for copy in copies + [item[0] for item in distant]:
        copy.wait_send()
    for copy in passed:
        copy.wait()


def gather_tp(blocks, spread, number):
    size, tp = blocks.shape[0], lax.axis_size("tp")
    pairs = tp // PAIR
    return pl.pallas_call(
        functools.partial(gather_kernel, size, pairs, spread),
        out_shape=jax.ShapeDtypeStruct((tp,) + blocks.shape, blocks.dtype),
        in_specs=[VMEM],
        out_specs=VMEM,
        scratch_shapes=[pltpu.SemaphoreType.DMA((size,))] * 2
        + [pltpu.SemaphoreType.DMA((pairs, size))] * 4,
        compiler_params=pltpu.CompilerParams(collective_id=number, has_side_effects=True),
    )(blocks)


def reduce_kernel(size, pairs, spread, source, target, near, paired, arrived, *rest):
    done = rest[0] if spread else None
    sems = rest[1:] if spread else rest
    pair_sems, far_sems, sp_sems = sems[:2], sems[2:4], sems[4:]
    me = lax.axis_index("sp")
    sibling = {"tp": tp_member(0, True)}
    far = [{"tp": tp_member(across, False)} for across in range(1, pairs)]
    peers = [group_member("sp", size, step) for step in range(1, size)] if spread else []
    greet([peer[2] for peer in peers] + [sibling] + far)
    order = [lax.rem(me + k + 1, size) if spread else k for k in range(size)]
    hops = list(range(1, pairs)) + [0]
    first = {}
    for k in range(size):
        for across in hops:
            copy = remote(
                source.at[tp_member(across, True), order[k]],
                near.at[across, order[k]],
                pair_sems,
                (across, k),
                sibling,
            )
            copy.start()
            first[k, across] = copy
    second = {}
    for k in range(size):
        for across in hops:
            first[k, across].wait_recv()
            total = source[tp_member(across, False), order[k]].astype(jnp.float32)
            total = total + near[across, order[k]].astype(jnp.float32)
            paired[across, order[k]] = total.astype(paired.dtype)
        for across in range(1, pairs):
            copy = remote(
                paired.at[across, order[k]],
                arrived.at[across, order[k]],
                far_sems,
                (across, k),
                far[across - 1],
            )
            copy.start()
            second[k, across] = copy
    third = []
    for k in range(size):
        total = paired[0, order[k]].astype(jnp.float32)
        for across in range(1, pairs):
            second[k, across].wait_recv()
            total = total + arrived[across, order[k]].astype(jnp.float32)
        if not spread:
            target[order[k]] = total
        elif k == size - 1:
            target[me] = total.astype(target.dtype)
        else:
            done[order[k]] = total.astype(done.dtype)
            copy = remote(done.at[order[k]], target.at[me], sp_sems, k, peers[k][2])
            copy.start()
            third.append(copy)
    for copy in list(first.values()) + list(second.values()):
        copy.wait_send()
    for copy in third:
        copy.wait()


def reduce_tp(blocks, spread, number):
    tp, size, rows, width = blocks.shape
    pairs = tp // PAIR
    kept = pltpu.VMEM((pairs, size, rows, width), jnp.bfloat16)
    done = [pltpu.VMEM((size, rows, width), jnp.bfloat16)] if spread else []
    return pl.pallas_call(
        functools.partial(reduce_kernel, size, pairs, spread),
        out_shape=jax.ShapeDtypeStruct(
            (size, rows, width), jnp.bfloat16 if spread else jnp.float32
        ),
        in_specs=[VMEM],
        out_specs=VMEM,
        scratch_shapes=[kept] * 3
        + done
        + [pltpu.SemaphoreType.DMA((pairs, size))] * 4
        + [pltpu.SemaphoreType.DMA((size,))] * 2,
        compiler_params=pltpu.CompilerParams(collective_id=number, has_side_effects=True),
    )(blocks)


def local_pass(queries, key_rows, values, decay_factors, key_width, value_width):
    count_of_tokens = queries.shape[0]
    head_count = queries.shape[1] // key_width
    blocks = count_of_tokens // BLK
    lower = jnp.tril(jnp.ones((BLK, BLK), jnp.float32))

    def arrange(source, feature_channels):
        return (
            source.astype(jnp.float32)
            .reshape(blocks, BLK, head_count, feature_channels)
            .transpose(0, 2, 1, 3)
        )

    query_blocks = arrange(queries, key_width) * key_width ** (-0.5)
    key_blocks = arrange(key_rows, key_width)
    value_blocks = arrange(values, value_width)
    cumulative = jnp.einsum("ts,nhsd->nhtd", lower, arrange(decay_factors, key_width), precision=highest)
    block_end = cumulative[:, :, -1:, :]
    query_decayed = query_blocks * jnp.exp(cumulative)
    key_inverse = key_blocks * jnp.exp(-cumulative)
    key_to_end = key_blocks * jnp.exp(block_end - cumulative)
    scores = jnp.einsum("nhtd,nhsd->nhts", query_decayed, key_inverse, precision=highest) * lower
    inner = jnp.einsum("nhts,nhsv->nhtv", scores, value_blocks, precision=highest)
    added = jnp.einsum("nhsd,nhsv->nhdv", key_to_end, value_blocks, precision=highest)
    state = jnp.zeros((head_count, key_width, value_width), jnp.float32)
    states = []
    for n in range(blocks):
        states.append(state)
        state = jnp.exp(block_end[n, :, 0])[:, :, None] * state + added[n]
    ends = block_end[:, :, 0]
    return (query_decayed, inner, jnp.stack(states), ends, state)


def finish_pass(query_decayed, inner, states, ends, entering):
    before = jnp.cumsum(ends, axis=0) - ends
    states = states + jnp.exp(before)[:, :, :, None] * entering[None]
    out = inner + jnp.einsum("nhtd,nhdv->nhtv", query_decayed, states, precision=highest)
    blocks, heads, rows, width = out.shape
    return out.transpose(0, 2, 1, 3).reshape(blocks * rows, heads, width)


def entering_state(totals, states, index):
    size = totals.shape[0]
    k = jnp.arange(size)
    reached = (k < index)[:, None]
    masked = jnp.where(reached, totals, 0.0)
    after = (k[None, :] > k[:, None]).astype(jnp.float32)
    behind = jnp.sum(after[:, :, None] * masked[None], axis=1)
    factor = jnp.where(reached, jnp.exp(behind), 0.0)
    return jnp.sum(factor[:, :, None] * states.astype(jnp.float32), axis=0)


def head_norm(attention, head_gain, gate):
    inverse_rms = lax.rsqrt(jnp.mean(attention * attention, axis=-1, keepdims=True) + epsilon)
    gate_silu = jax.nn.silu(gate.astype(jnp.float32).reshape(attention.shape))
    mixed_rows = attention * inverse_rms * head_gain * gate_silu
    return mixed_rows.astype(jnp.bfloat16).reshape(attention.shape[0], -1)


def rms_scale(residual, gain_vector):
    as_float = residual.astype(jnp.float32)
    inverse_rms = lax.rsqrt(jnp.mean(as_float * as_float, axis=-1, keepdims=True) + epsilon)
    return (as_float * inverse_rms * gain_vector).astype(jnp.bfloat16)


def route_positions(block_routes, experts):
    flattened = block_routes.reshape(-1)
    amount = flattened.shape[0]
    onehot = flattened[:, None] == jnp.arange(experts, dtype=jnp.int32)[None, :]
    earlier = jnp.tril(jnp.ones((amount, amount), jnp.bfloat16), -1)
    before = jnp.dot(earlier, onehot.astype(jnp.bfloat16), preferred_element_type=jnp.float32)
    ranking = jnp.sum(jnp.where(onehot, before, 0.0), axis=1).astype(jnp.int32)
    return ranking.reshape(block_routes.shape)


def shards(
    query_first,
    key_first,
    value_first,
    decay_first,
    gate_first,
    norm_first,
    proj_first,
    query_second,
    key_second,
    value_second,
    decay_second,
    gate_second,
    norm_second,
    proj_second,
    residual_in,
    expert_norm,
    route_ids,
    route_weight,
    expert_gate,
    expert_up,
    expert_down,
):
    sp_size, tp_size = lax.axis_size("sp"), lax.axis_size("tp")
    sp_index, tp_index = lax.axis_index("sp"), lax.axis_index("tp")
    first = local_pass(query_first, key_first, value_first, decay_first, KA, VA)
    second = local_pass(query_second, key_second, value_second, decay_second, KB, VB)
    total_first = jnp.sum(first[3], axis=0).reshape(1, -1)
    total_second = jnp.sum(second[3], axis=0).reshape(1, -1)
    totals = jnp.concatenate((total_first, total_second), axis=1)
    totals = jnp.broadcast_to(totals, (8, totals.shape[1]))
    all_totals, all_first, all_second, *columns = exchange(
        (
            totals,
            first[4].reshape(-1, VA).astype(jnp.bfloat16),
            second[4].reshape(-1, VB).astype(jnp.bfloat16),
            proj_first,
            proj_second,
        ),
        "sp",
        sp_size,
        False,
        0,
    )
    columns = [part.transpose(1, 0, 2).reshape(part.shape[1], -1) for part in columns]
    projection = jnp.concatenate(columns, axis=0)
    cut = total_first.shape[1]
    enter_first = entering_state(all_totals[:, 0, :cut], all_first, sp_index)
    enter_second = entering_state(all_totals[:, 0, cut:], all_second, sp_index)
    attention_first = finish_pass(*first[:4], enter_first.reshape(first[4].shape))
    attention_second = finish_pass(*second[:4], enter_second.reshape(second[4].shape))
    mixed_first = head_norm(attention_first, norm_first, gate_first)
    mixed_second = head_norm(attention_second, norm_second, gate_second)
    mixed_rows = jnp.concatenate((mixed_first, mixed_second), axis=1)
    partial_terms = jnp.dot(mixed_rows, projection, preferred_element_type=jnp.float32)
    block_tokens, top_count = route_ids.shape
    model_width = partial_terms.shape[1]
    own_tokens = block_tokens // tp_size
    by_owner = (tp_size, PAIR, own_tokens // PAIR, model_width)
    mixture = reduce_tp(partial_terms.astype(jnp.bfloat16).reshape(by_owner), False, 1)
    mixture = mixture.reshape(own_tokens, model_width)
    residual = (residual_in.astype(jnp.float32) + mixture).astype(jnp.bfloat16)
    normed = rms_scale(residual, expert_norm)
    gathered = gather_tp(normed.reshape(by_owner[1:]), False, 2)
    gathered = gathered.reshape(block_tokens, model_width)

    experts = sp_size
    capacity = 2 * top_count * block_tokens // experts
    quarter = capacity // tp_size
    slots = experts * quarter
    place = route_positions(route_ids, experts) - tp_index * quarter
    local = jnp.where((place >= 0) & (place < quarter), route_ids * quarter + place, -1)
    numbers = jnp.arange(slots, dtype=jnp.int32)
    chosen, weights = (False, 0.0)
    for c in range(top_count):
        chosen = chosen | (numbers[:, None] == local[None, :, c])
        weights = weights + jnp.where(
            numbers[None, :] == local[:, c, None], route_weight[:, c, None], 0.0
        )
    outgoing = jnp.dot(
        chosen.astype(jnp.bfloat16), gathered, preferred_element_type=jnp.float32
    ).astype(jnp.bfloat16)
    incoming = gather_tp(outgoing.reshape(experts, quarter, model_width), True, 3)
    incoming = incoming.reshape(-1, model_width)
    gate_part = jnp.dot(incoming, expert_gate[0], preferred_element_type=jnp.float32)
    up_part = jnp.dot(incoming, expert_up[0], preferred_element_type=jnp.float32)
    hidden = (jax.nn.silu(gate_part) * up_part).astype(jnp.bfloat16)
    produced = jnp.dot(hidden, expert_down[0], preferred_element_type=jnp.float32)
    produced = produced.astype(jnp.bfloat16).reshape(tp_size, experts, quarter, model_width)
    returned = reduce_tp(produced, True, 4)
    returned = returned.reshape(slots, model_width)
    coarse = weights.astype(jnp.bfloat16)
    fine = (weights - coarse.astype(jnp.float32)).astype(jnp.bfloat16)
    weighted = jnp.dot(coarse, returned, preferred_element_type=jnp.float32)
    weighted = weighted + jnp.dot(fine, returned, preferred_element_type=jnp.float32)
    combined = reduce_tp(weighted.astype(jnp.bfloat16).reshape(by_owner), False, 5)
    combined = combined.reshape(own_tokens, model_width)
    return (residual.astype(jnp.float32) + combined).astype(jnp.bfloat16)


def solution(mesh):
    in_specs = (
        P("sp", "tp"),
        P("sp", "tp"),
        P("sp", "tp"),
        P("sp", "tp"),
        P("sp", "tp"),
        P(),
        P("tp", "sp"),
        P("sp", "tp"),
        P("sp", "tp"),
        P("sp", "tp"),
        P("sp", "tp"),
        P("sp", "tp"),
        P(),
        P("tp", "sp"),
        P(("sp", "tp"), None),
        P(),
        P("sp", None),
        P("sp", None),
        P("sp", None, "tp"),
        P("sp", None, "tp"),
        P("sp", "tp", None),
    )
    out_specs = P(("sp", "tp"), None)
    return jax.shard_map(shards, mesh=mesh, in_specs=in_specs, out_specs=out_specs, check_vma=False)
```
